32 devices in a mesh: rep: 2 (over x), fs: 8 (over z, y), tp: 2 (over core).
Axes of the slice: x: 2, y: 2, z: 4, core: 2. Of those that a mesh axis runs over, the one named last changes fastest.
Arguments:
- stream: bfloat16 [16, 1024, 2048], P(('rep', 'fs'), None, 'tp'), may hold values from -6 to 6
- norm_gain: float32 [2048], replicated, may hold values from 0.1 to 1.9
- w_in: float32 [2048, 512], P('fs', 'tp'), may hold values from -0.125 to 0.125
- s_in: float32 [512], P(('tp', 'fs')), may hold values from 0.1 to 1.9
- pool_w: bfloat16 [4, 128, 128], replicated, may hold values from -0.5 to 0.5
- w_out: float32 [512, 2048], P('fs', 'tp'), may hold values from -0.25 to 0.25
- s_out: float32 [2048], P(('tp', 'fs')), may hold values from 0.1 to 1.9
- ffn_gain: float32 [2048], replicated, may hold values from 0.1 to 1.9
- w_up: float32 [2048, 8192], P('fs', 'tp'), may hold values from -0.125 to 0.125
- s_up: float32 [8192], P(('tp', 'fs')), may hold values from 0.1 to 1.9
- w_down: float32 [8192, 2048], P('tp', 'fs'), may hold values from -0.0625 to 0.0625
- s_down: float32 [2048], P('fs'), may hold values from 0.1 to 1.9
Outputs:
- result: bfloat16 [16, 1024, 2048], P(('rep', 'fs'), None, 'tp')
The draws below stay inside these ranges and needn't reach their ends.
All inputs are finite; a program needn't handle non-finite values.
Results may differ from the reference program's by a relative error of at most 0.012.
Values may be sent and summed in bfloat16 or wider, within the bound.
A program may use at most 128 MiB of HBM per device.

```python
import jax
import jax.numpy as jnp
from jax import lax

D = 2048
FF = 8192
PW = 512
GROUP = 128
SEQ_LEN = 1024
BATCH = 16
N_TP = 2


def block_scale(stream_key, shape, cuts, least, top_value):
    level, own = 1.0, jax.random.fold_in(stream_key, 6)
    for axis_at, shards_of in cuts:
        draws = jnp.exp(jax.random.uniform(jax.random.fold_in(own, axis_at), (shards_of,), jnp.float32, least / len(cuts), top_value / len(cuts)))
        level = level * jnp.repeat(draws, shape[axis_at] // shards_of).reshape([-1 if axis == axis_at else 1 for axis in range(len(shape))])
    return level


def bell_draw(key, shape, scale, limit, shards=(), kind=jnp.bfloat16):
    entries = jax.random.normal(key, shape, jnp.float32) * scale
    if len(shards) > 0:
        entries = block_scale(key, shape, shards, -0.22, 0.18) * entries
    return jnp.clip(entries, min=-limit, max=limit).astype(kind)


def setup_inputs(seed: int = 0) -> dict:
    key_list = jax.random.split(jax.random.key(seed), 13)
    return {
        "stream": bell_draw(key_list[0], (BATCH, SEQ_LEN, D), 1.0, 6.0, ((0, 16), (2, 2))),
        "norm_gain": jnp.clip(1.0 + 0.18 * jax.random.normal(key_list[1], (D,), jnp.float32), 0.1, 1.9),
        "w_in": bell_draw(key_list[2], (D, PW), D ** -0.5, 0.125, ((0, 8), (1, 2)), jnp.float32),
        "s_in": jnp.clip(1.0 + 0.18 * jax.random.normal(key_list[3], (PW,), jnp.float32), 0.1, 1.9),
        "pool_w": bell_draw(key_list[4], (4, GROUP, GROUP), GROUP ** -0.5, 0.5),
        "w_out": bell_draw(key_list[5], (PW, D), PW ** -0.5, 0.25, ((0, 8), (1, 2)), jnp.float32),
        "s_out": jnp.clip(1.0 + 0.18 * jax.random.normal(key_list[6], (D,), jnp.float32), 0.1, 1.9),
        "ffn_gain": jnp.clip(1.0 + 0.18 * jax.random.normal(key_list[7], (D,), jnp.float32), 0.1, 1.9),
        "w_up": bell_draw(key_list[8], (D, FF), D ** -0.5, 0.125, ((0, 8), (1, 2)), jnp.float32),
        "s_up": jnp.clip(1.0 + 0.18 * jax.random.normal(key_list[9], (FF,), jnp.float32), 0.1, 1.9),
        "w_down": bell_draw(key_list[10], (FF, D), FF ** -0.5, 0.0625, ((0, 2), (1, 8)), jnp.float32),
        "s_down": jnp.clip(1.0 + 0.18 * jax.random.normal(key_list[11], (D,), jnp.float32), 0.1, 1.9),
    }


epsilon = 0.25

def rms_rows(values, gain):
    floats = values.astype(jnp.float32)
    scale = lax.rsqrt(lax.optimization_barrier(jnp.mean(floats * floats, axis=-1, keepdims=True)) + epsilon)
    return (floats * scale * gain).astype(jnp.bfloat16)

def pool_sequence(pool_in):
    length = pool_in.shape[0]
    floats = pool_in.astype(jnp.float32)
    running = jnp.concatenate([jnp.zeros((1, floats.shape[1]), jnp.float32), jnp.cumsum(floats, axis=0)], axis=0)
    positions = jnp.arange(length, dtype=jnp.int32)
    pieces = []
    for level in range(4):
        half = 2 ** level
        lower = jnp.clip(positions - half, 0, length).astype(jnp.int32)
        upper = jnp.clip(positions + half, 0, length).astype(jnp.int32)
        part = running[:, level * GROUP:(level + 1) * GROUP]
        counts = (upper - lower).astype(jnp.float32)[:, None]
        pieces.append((part[upper] - part[lower]) / counts - floats[:, level * GROUP:(level + 1) * GROUP])
    return jnp.concatenate(pieces, axis=1).astype(jnp.bfloat16)

def one_sequence(tokens, norm_gain, w_in, s_in, pool_w, w_out, s_out, ffn_gain, w_up, s_up, w_down, s_down):
    length = tokens.shape[0]
    normed = rms_rows(tokens, norm_gain)
    pool_in = (jnp.dot(normed, w_in.astype(jnp.bfloat16), preferred_element_type=jnp.float32) * s_in).astype(jnp.bfloat16)
    pooled = pool_sequence(pool_in)
    grouped = jnp.einsum('lgc,gcd->lgd', pooled.reshape(length, 4, GROUP).astype(jnp.float32), pool_w.astype(jnp.float32))
    grouped = grouped.reshape(length, PW).astype(jnp.bfloat16)
    branch = jnp.dot(grouped, w_out.astype(jnp.bfloat16), preferred_element_type=jnp.float32) * s_out
    mixed = (tokens.astype(jnp.float32) + branch).astype(jnp.bfloat16)
    ffn_in = rms_rows(mixed, ffn_gain)
    upward = jnp.dot(ffn_in, w_up.astype(jnp.bfloat16), preferred_element_type=jnp.float32) * s_up
    hidden = jnp.square(jax.nn.relu(upward)).astype(jnp.bfloat16)
    block = FF // N_TP
    hidden_blocks = hidden.reshape(length, N_TP, block).astype(jnp.float32)
    down_blocks = w_down.astype(jnp.bfloat16).reshape(N_TP, block, D).astype(jnp.float32)
    partials = jnp.einsum('ljf,jfd->jld', hidden_blocks, down_blocks) * s_down
    rounded = lax.optimization_barrier(partials.astype(jnp.bfloat16))
    summed = lax.optimization_barrier(jnp.sum(rounded.astype(jnp.float32), axis=0))
    return (mixed.astype(jnp.float32) + summed).astype(jnp.bfloat16)

def reference(stream, norm_gain, w_in, s_in, pool_w, w_out, s_out, ffn_gain, w_up, s_up, w_down, s_down):

    def single(tokens):
        return one_sequence(tokens, norm_gain, w_in, s_in, pool_w, w_out, s_out, ffn_gain, w_up, s_up, w_down, s_down)
    return lax.map(single, stream)
```

```python
import jax
import jax.numpy as jnp
from jax import lax
from jax.sharding import PartitionSpec as P

GROUP = 128


epsilon = 0.25
bf16 = jnp.bfloat16
f32 = jnp.float32


def dot(left, right):
    return jnp.dot(left, right, preferred_element_type=f32)


def rms_rows(values, gain):
    floats = values.astype(f32)
    scale = lax.rsqrt(jnp.mean(floats * floats, axis=-1, keepdims=True) + epsilon)
    return (floats * scale * gain).astype(bf16)


def shifted(value, axis_name, count, offset):
    return lax.ppermute(value, axis_name, [(i, (i + offset) % count) for i in range(count)])


def swap_gather(value, axis_name, count, axis):
    index = lax.axis_index(axis_name)
    width = value.shape[axis]
    shape = list(value.shape)
    shape[axis] = width * count
    if count == 2:
        other = shifted(value, axis_name, count, 1)
        low = jnp.where(index == 0, value, other)
        high = jnp.where(index == 0, other, value)
        return jnp.concatenate([low, high], axis=axis)
    full = jnp.zeros(shape, value.dtype)
    full = lax.dynamic_update_slice_in_dim(full, value, index * width, axis)
    for offset in range(1, count):
        piece = shifted(value, axis_name, count, offset)
        origin = (index - offset) % count
        full = lax.dynamic_update_slice_in_dim(full, piece, origin * width, axis)
    return full


def fs_sent(value, factors, offset_a, offset_b):
    n_a, n_b = factors
    pairs = []
    for i in range(n_a * n_b):
        pairs.append((i, ((i // n_b) ^ offset_a) * n_b + ((i % n_b) ^ offset_b)))
    return lax.ppermute(value, "fs", pairs)


def fs_pieces(value, factors):
    n_a, n_b = factors
    rows = [[value] for _ in range(n_a)]
    for x in range(1, n_a):
        rows[x] = [fs_sent(value, factors, x, 0)]
    for y in range(1, n_b):
        for x in range(n_a):
            rows[x].append(fs_sent(rows[x][0], factors, 0, y))
    return rows


def fs_origin(factors, x, y):
    index = lax.axis_index("fs")
    return ((index // factors[1]) ^ x) * factors[1] + ((index % factors[1]) ^ y)


def placed(rows, factors):
    block = rows[0][0].shape[0]
    width = rows[0][0].shape[1]
    full = jnp.zeros((block * factors[0] * factors[1], width), rows[0][0].dtype)
    for y in range(factors[1]):
        for x in range(factors[0]):
            full = lax.dynamic_update_slice_in_dim(
                full, rows[x][y], fs_origin(factors, x, y) * block, 0
            )
    return full


def pool_local(pool_in, first):
    length, width = pool_in.shape
    positions = jnp.arange(length, dtype=jnp.int32)
    source = positions[None, :]
    target = positions[:, None]
    group_of = (first + jnp.arange(width, dtype=jnp.int32)) // GROUP
    means = jnp.zeros((length, width), f32)
    for level in range(4):
        half = 2**level
        band_ones = ((source >= target - half) & (source < target + half)).astype(bf16)
        counts = (jnp.minimum(positions + half, length) - jnp.maximum(positions - half, 0)).astype(f32)
        sums = dot(band_ones, pool_in) / counts[:, None]
        means = jnp.where(group_of[None, :] == level, sums, means)
    return (means - pool_in.astype(f32)).astype(bf16)


def on_device(
    n_rep, n_fs, n_tp,
    stream, norm_gain, w_in, s_in, pool_w, w_out, s_out, ffn_gain, w_up, s_up, w_down, s_down,
):
    rep = lax.axis_index("rep")
    tokens = stream[0]
    length, local_width = tokens.shape
    hidden_width = w_up.shape[1] // n_rep

    n_a = n_tp * max(1, 4 // n_tp)
    factors = (n_a, n_fs // n_a)

    scales = jnp.concatenate([s_in, s_out, s_up, s_down])[None]
    scale_rows = [
        [scales if x == y == 0 else fs_sent(scales, factors, x, y) for y in range(factors[1])]
        for x in range(n_a)
    ]
    scales = placed(scale_rows, factors)
    ends, at = [], 0
    for part in (s_in, s_out, s_up, s_down):
        ends.append(scales[:, at:at + part.shape[0]])
        at += part.shape[0]
    scale_in, scale_out, scale_up = (part.reshape(-1) for part in ends[:3])
    scale_down = ends[3]

    in_rows = fs_pieces(w_in.astype(bf16), factors)
    out_rows = fs_pieces(w_out.astype(bf16), factors)
    w_in_all = placed(in_rows, factors)
    w_out_all = placed(out_rows, factors)

    up_own = lax.dynamic_slice_in_dim(w_up, rep * hidden_width, hidden_width, 1).astype(bf16)
    up_rows = fs_pieces(up_own, factors)
    up_all = placed(up_rows, factors)
    down_own = lax.dynamic_slice_in_dim(w_down, rep * hidden_width, hidden_width, 0).astype(bf16)
    down_own, *_ = lax.optimization_barrier((down_own, *[in_rows[x][0] for x in range(1, n_a)]))
    down_rows = fs_pieces(down_own, factors)

    normed = rms_rows(swap_gather(tokens, "tp", n_tp, 1), norm_gain)
    pool_in = (dot(normed, w_in_all) * scale_in).astype(bf16)
    pooled = pool_local(pool_in, lax.axis_index("tp") * pool_in.shape[1])
    pooled_all = swap_gather(pooled, "tp", n_tp, 1)
    groups = pool_w.shape[0]
    grouped = jnp.einsum(
        "lgc,gcd->lgd", pooled_all.reshape(length, groups, GROUP), pool_w, preferred_element_type=f32
    ).reshape(length, groups * GROUP).astype(bf16)
    mixed = (tokens.astype(f32) + dot(grouped, w_out_all) * scale_out).astype(bf16)

    mixed_own = swap_gather(mixed, "tp", n_tp, 1)
    sequences = [mixed_own]
    for offset in range(1, n_rep):
        other = shifted(mixed, "rep", n_rep, offset)
        sequences.append(swap_gather(other, "tp", n_tp, 1))
    scale_hidden = lax.dynamic_slice_in_dim(scale_up, rep * hidden_width, hidden_width, 0)
    hidden = []
    for rows in sequences:
        rows = rms_rows(rows, ffn_gain)
        upward = dot(rows, up_all)
        hidden.append(jnp.square(jax.nn.relu(upward * scale_hidden)).astype(bf16))

    hidden = jnp.concatenate(hidden, axis=0)
    width = w_down.shape[1]
    per_tp = n_a // n_tp
    tp = lax.axis_index("tp")
    turn = ((lax.axis_index("fs") // factors[1]) // per_tp) ^ tp
    result = jnp.zeros((length, local_width), bf16)
    for y in range(factors[1]):
        for xi in range(per_tp):
            stacked = jnp.stack([down_rows[xt * per_tp + xi][y] for xt in range(n_tp)])
            blocks, block_scales = [], []
            for k in range(n_tp):
                blocks.append(lax.dynamic_index_in_dim(stacked, turn ^ k, 0, keepdims=False))
                origin = fs_origin(factors, xi, y) ^ ((turn ^ k) * per_tp * factors[1])
                block_scales.append(lax.dynamic_index_in_dim(scale_down, origin, 0, keepdims=False))
            both = jnp.concatenate(blocks, axis=1)
            partial = (dot(hidden, both) * jnp.concatenate(block_scales)).astype(bf16)
            total = partial[:, :width].astype(f32)
            for k in range(1, n_tp):
                pairs = [(i, i ^ k) for i in range(n_tp)]
                total = total + lax.ppermute(partial[:, k * width:(k + 1) * width], "tp", pairs).astype(f32)
            own = total[:length]
            for k in range(1, n_rep):
                back = shifted(total[k * length:(k + 1) * length].astype(bf16), "rep", n_rep, -k)
                own = own + back.astype(f32)
            inner = (fs_origin(factors, xi, y) % (per_tp * factors[1])) * width
            mixed_part = lax.dynamic_slice_in_dim(mixed, inner, width, 1)
            piece = (mixed_part.astype(f32) + own).astype(bf16)
            result = lax.dynamic_update_slice_in_dim(result, piece, inner, 1)
    return result[None]


def solution(mesh):
    n_rep, n_fs, n_tp = (mesh.shape[name] for name in ("rep", "fs", "tp"))

    def body(*args):
        return on_device(n_rep, n_fs, n_tp, *args)

    return jax.shard_map(
        body,
        mesh=mesh,
        in_specs=(
            P(("rep", "fs"), None, "tp"),
            P(),
            P("fs", "tp"),
            P(("tp", "fs")),
            P(),
            P("fs", "tp"),
            P(("tp", "fs")),
            P(),
            P("fs", "tp"),
            P(("tp", "fs")),
            P("tp", "fs"),
            P("fs"),
        ),
        out_specs=P(("rep", "fs"), None, "tp"),
        check_vma=False,
    )
```
